32 devices in a mesh: sp: 16 (over z, y, x), dp: 2 (over core).
Axes of the slice: x: 2, y: 2, z: 4, core: 2. Of those that a mesh axis runs over, the one named last changes fastest.
Arguments:
- tokens: bfloat16 [2048, 2048], P('sp', 'dp'), may hold values from -6 to 6
- cotangent: bfloat16 [2048, 2048], P('sp', 'dp'), may hold values from -6 to 6
- in_weight: bfloat16 [256, 2048], P('sp', 'dp'), may hold values from -0.125 to 0.125
- out_weight: bfloat16 [256, 2048], P('sp', 'dp'), may hold values from -0.375 to 0.375
- decay_rate: float32 [16, 32], P('sp'), may hold values from 0 to 1
- frequency: float32 [16, 32], P('sp'), may hold values from 4 to 40
- step_log: float32 [16], P('sp'), may hold values from -2.6593 to -1.9661
- drive_real: float32 [16, 32, 16], P('sp'), may hold values from -6 to 6
- drive_imag: float32 [16, 32, 16], P('sp'), may hold values from -6 to 6
- readout_real_part: float32 [16, 16, 32], P('sp'), may hold values from -0.75 to 0.75
- readout_imaginary: float32 [16, 16, 32], P('sp'), may hold values from -0.75 to 0.75
- skip_gain: float32 [16, 16], P('sp'), may hold values from -4 to 4
Outputs:
- grad_tokens: bfloat16 [2048, 2048], P('sp', 'dp')
- grad_in_weight: float32 [256, 2048], P('sp', 'dp')
- grad_out_weight: float32 [256, 2048], P('sp', 'dp')
The draws below stay inside these ranges and needn't reach their ends.
All inputs are finite; a program needn't handle non-finite values.
Results may differ from the reference program's by a relative error of at most 0.02.
Values may be sent and summed in bfloat16 or wider, within the bound.
A program may use at most 64 MiB of HBM per device.

```python
import math
import jax
import jax.numpy as jnp
from jax import lax

D = 2048
C = 16
P_SIZE = 32
GROUPS = 16
DSSM = 256
LENGTH = 2048
N_DP = 2


def draw_decay_rate(key, part):
    own_key = jax.random.fold_in(key, 5)
    pick_key, slow_key, fast_key = jax.random.split(own_key, 3)
    slow_share = 0.5
    chooser = jax.random.uniform(pick_key, (GROUPS, P_SIZE), jnp.float32)
    slow_value = jax.random.uniform(slow_key, (GROUPS, P_SIZE), jnp.float32, math.log(0.07), math.log(0.1))
    fast_value = jax.random.uniform(fast_key, (GROUPS, P_SIZE), jnp.float32, math.log(0.3), math.log(0.6))
    return jnp.exp(jnp.where(chooser < slow_share, slow_value, fast_value)).astype(jnp.float32)


def position_envelope(key):
    block_count = (LENGTH + 15) // 16
    loud = jax.random.uniform(key, (block_count,), jnp.float32) < 0.25
    levels = jnp.where(loud, 1.0, 0.15).astype(jnp.float32)
    return jnp.repeat(levels, 16)[:LENGTH]


def enveloped_rows(key):
    level_key, value_key = jax.random.split(key)
    values = jax.random.truncated_normal(value_key, -6.0, 6.0, (LENGTH, D), jnp.float32)
    return (values * position_envelope(level_key)[:, None]).astype(jnp.bfloat16)


def draw_tokens(key, part):
    return enveloped_rows(jax.random.fold_in(key, 11))


def draw_cotangent(key, part):
    return enveloped_rows(jax.random.fold_in(key, 23))


def steps_of(stream_key, dims, cuts, least, largest):
    factor_of = 1.0
    for axis_at, shards_of in cuts:
        draws = jax.random.uniform(jax.random.fold_in(jax.random.fold_in(stream_key, 6), axis_at), (shards_of,), jnp.float32, least / len(cuts), largest / len(cuts))
        factor_of = factor_of * jnp.repeat(jnp.exp(draws), dims[axis_at] // shards_of).reshape((-1,) + (1,) * (len(dims) - 1 - axis_at))
    return factor_of


def normal_values(rng, dims, scale, limit, cuts=(), held_as=jnp.bfloat16):
    loudness = steps_of(rng, dims, cuts, -0.22, 0.18) if cuts else 1.0
    result = jax.random.normal(rng, dims, jnp.float32) * scale * loudness
    return jnp.minimum(jnp.maximum(result, -limit), limit).astype(held_as)


def setup_inputs(seed: int = 0) -> dict:
    keys = jax.random.split(jax.random.key(seed), 13)
    return {
        "tokens": draw_tokens(jax.random.fold_in(keys[12], 71), 0),
        "cotangent": draw_cotangent(jax.random.fold_in(keys[12], 71), 0),
        "in_weight": normal_values(keys[2], (DSSM, D), D ** -0.5, 0.125, ((0, 16), (1, 2))),
        "out_weight": normal_values(keys[3], (DSSM, D), DSSM ** -0.5, 0.375, ((0, 16), (1, 2))),
        "decay_rate": draw_decay_rate(jax.random.fold_in(keys[12], 71), 0),
        "frequency": jnp.clip(4.0 + 36.0 * jax.random.uniform(keys[5], (GROUPS, P_SIZE), jnp.float32) ** steps_of(keys[5], (GROUPS, P_SIZE), ((0, 16),), -0.2, 0.2), 4.0, 40.0),
        "step_log": jnp.clip(-2.6593 + 0.6932001 * jax.random.uniform(keys[6], (GROUPS,), jnp.float32) ** steps_of(keys[6], (GROUPS,), ((0, 16),), -0.2, 0.2), -2.6593, -1.9661),
        "drive_real": normal_values(keys[7], (GROUPS, P_SIZE, C), 0.6, 6.0, ((0, 16),), jnp.float32),
        "drive_imag": normal_values(keys[8], (GROUPS, P_SIZE, C), 0.6, 6.0, ((0, 16),), jnp.float32),
        "readout_real_part": normal_values(keys[9], (GROUPS, C, P_SIZE), (2 * P_SIZE) ** -0.5, 0.75, ((0, 16),), jnp.float32),
        "readout_imaginary": normal_values(keys[10], (GROUPS, C, P_SIZE), (2 * P_SIZE) ** -0.5, 0.75, ((0, 16),), jnp.float32),
        "skip_gain": normal_values(keys[11], (GROUPS, C), 0.3, 4.0, ((0, 16),), jnp.float32),
    }


finest_precision = lax.Precision.HIGHEST

def combine(earlier, later):
    first_real, first_imag, first_sum_real, first_sum_imag = earlier
    next_real, next_imag, next_sum_real, next_sum_imag = later
    return (first_real * next_real - first_imag * next_imag, first_real * next_imag + first_imag * next_real, next_real * first_sum_real - next_imag * first_sum_imag + next_sum_real, next_real * first_sum_imag + next_imag * first_sum_real + next_sum_imag)

def discretize(decay_rate, frequency, step_log, drive_real, drive_imag):
    step_size = jnp.exp(step_log)[..., None]
    magnitude = jnp.exp(-decay_rate * step_size)
    angle = frequency * step_size
    decay_real = magnitude * jnp.cos(angle)
    decay_imag = magnitude * jnp.sin(angle)
    modulus = decay_rate * decay_rate + frequency * frequency
    hold_real = (-decay_rate * (decay_real - 1.0) + frequency * decay_imag) / modulus
    hold_imag = (-frequency * (decay_real - 1.0) - decay_rate * decay_imag) / modulus
    input_real = hold_real[..., None] * drive_real - hold_imag[..., None] * drive_imag
    input_imag = hold_real[..., None] * drive_imag + hold_imag[..., None] * drive_real
    return (decay_real, decay_imag, input_real, input_imag)

def one_group(inputs):
    drive_rows, back_rows, decay_rate, frequency, step_log, drive_real, drive_imag, readout_real_part, readout_imaginary, skip_gain = inputs
    decay_real, decay_imag, input_real, input_imag = discretize(decay_rate, frequency, step_log, drive_real, drive_imag)
    length = drive_rows.shape[1]
    factor_real = jnp.broadcast_to(decay_real[:, None], (decay_real.shape[0], length))
    factor_imag = jnp.broadcast_to(decay_imag[:, None], (decay_imag.shape[0], length))
    push_real = jnp.einsum('pc,ck->pk', input_real, drive_rows, precision=finest_precision)
    push_imag = jnp.einsum('pc,ck->pk', input_imag, drive_rows, precision=finest_precision)
    _, _, state_real, state_imag = lax.associative_scan(combine, (factor_real, factor_imag, push_real, push_imag), axis=1)
    mixed_rows = jnp.einsum('cp,pk->ck', readout_real_part, state_real, precision=finest_precision) - jnp.einsum('cp,pk->ck', readout_imaginary, state_imag, precision=finest_precision) + skip_gain[:, None] * drive_rows
    gated, pullback = jax.vjp(jax.nn.gelu, mixed_rows)
    interior_gradient, = pullback(back_rows)
    pulled_real_part = jnp.einsum('cp,ck->pk', readout_real_part, interior_gradient, precision=finest_precision)[:, ::-1]
    pulled_imaginary = -jnp.einsum('cp,ck->pk', readout_imaginary, interior_gradient, precision=finest_precision)[:, ::-1]
    _, _, adjoint_real, adjoint_imag = lax.associative_scan(combine, (factor_real, -factor_imag, pulled_real_part, pulled_imaginary), axis=1)
    adjoint_real = adjoint_real[:, ::-1]
    adjoint_imag = adjoint_imag[:, ::-1]
    grad_rows = jnp.einsum('pc,pk->ck', input_real, adjoint_real, precision=finest_precision) + jnp.einsum('pc,pk->ck', input_imag, adjoint_imag, precision=finest_precision) + skip_gain[:, None] * interior_gradient
    return (grad_rows.astype(jnp.bfloat16), gated.astype(jnp.bfloat16))

def reference(tokens, cotangent, in_weight, out_weight, decay_rate, frequency, step_log, drive_real, drive_imag, readout_real_part, readout_imaginary, skip_gain):
    block_width = D // N_DP
    drive_sum = jnp.zeros((DSSM, LENGTH), jnp.float32)
    back_sum = jnp.zeros((DSSM, LENGTH), jnp.float32)
    for column_block in range(N_DP):
        low = column_block * block_width
        token_cols = tokens[:, low:low + block_width]
        cot_cols = cotangent[:, low:low + block_width]
        part_drive = jnp.dot(in_weight[:, low:low + block_width], token_cols.T, preferred_element_type=jnp.float32)
        part_back = jnp.dot(out_weight[:, low:low + block_width], cot_cols.T, preferred_element_type=jnp.float32)
        drive_sum = drive_sum + lax.optimization_barrier(part_drive.astype(jnp.bfloat16)).astype(jnp.float32)
        back_sum = back_sum + lax.optimization_barrier(part_back.astype(jnp.bfloat16)).astype(jnp.float32)
    projected = drive_sum.astype(jnp.bfloat16)
    back_mix = back_sum.astype(jnp.bfloat16)
    drive_groups = projected.astype(jnp.float32).reshape(GROUPS, C, LENGTH)
    back_groups = back_mix.astype(jnp.float32).reshape(GROUPS, C, LENGTH)
    grad_groups, gated_groups = lax.map(one_group, (drive_groups, back_groups, decay_rate, frequency, step_log, drive_real, drive_imag, readout_real_part, readout_imaginary, skip_gain))
    grad_mix = grad_groups.reshape(DSSM, LENGTH)
    gated = gated_groups.reshape(DSSM, LENGTH)
    grad_tokens = jnp.dot(grad_mix.T, in_weight, preferred_element_type=jnp.float32).astype(jnp.bfloat16)
    grad_scale = LENGTH ** (-0.5)
    grad_in_weight = jnp.dot(grad_mix, tokens, preferred_element_type=jnp.float32) * grad_scale
    grad_out_weight = jnp.dot(gated, cotangent, preferred_element_type=jnp.float32) * grad_scale
    return (grad_tokens, grad_in_weight, grad_out_weight)
```

```python
import functools

import jax
import jax.numpy as jnp
from jax import lax
from jax.experimental import pallas as pl
from jax.experimental.pallas import tpu as pltpu
from jax.sharding import PartitionSpec as P

MESH = pl.DeviceIdType.MESH
f32 = jnp.float32
bf16 = jnp.bfloat16
LANES = 128


def exact_dot(a, b):
    return jnp.dot(a, b, precision=lax.Precision.HIGHEST, preferred_element_type=f32)


def fast_dot(a, b):
    return jnp.dot(a, b, preferred_element_type=f32)


def dot_nt(a, b):
    return lax.dot_general(a, b, (((1,), (1,)), ((), ())), preferred_element_type=f32)


def dot_tn(a, b):
    return lax.dot_general(a, b, (((0,), (0,)), ((), ())), preferred_element_type=f32)


def kernel(
    sizes,
    tok_ref,
    cot_ref,
    inw_ref,
    outw_ref,
    pack_ref,
    gt_ref,
    giw_ref,
    gow_ref,
    win,
    wout,
    packs,
    btab,
    ctab,
    steps,
    pows,
    skips,
    dps,
    dpr,
    ends_out,
    ends,
    rsb,
    rsr,
    zs,
    zr,
    sz,
    rz,
    sq,
    rq,
    spk,
    rpk,
    sdp,
    rdp,
    sen,
    ren,
    srs,
    rrs,
    szs,
    rzs,
):
    n, nd, n_out, n_in, states, chans, n_groups = sizes
    length = tok_ref.shape[0]
    rows, width = inw_ref.shape
    n_packs = packs.shape[0]
    total_states = n_groups * states
    own_chans = n_groups * chans
    halves = total_states // LANES
    s = lax.axis_index("sp")
    d = lax.axis_index("dp")
    a = s // n_in
    q = lax.rem(s, n_in)

    def remote(src, dst, ssem, rsem, sp, dp):
        return pltpu.make_async_remote_copy(
            src_ref=src,
            dst_ref=dst,
            send_sem=ssem,
            recv_sem=rsem,
            device_id=(sp, dp),
            device_id_type=MESH,
        )

    def outer_at(k):
        return lax.rem(a + k + n_out, n_out)

    def inner_at(j):
        return lax.rem(q + j + n_in, n_in)

    barrier = pltpu.get_barrier_semaphore()
    for k in range(1, n):
        pl.semaphore_signal(barrier, inc=1, device_id=(lax.rem(s + k, n), d), device_id_type=MESH)
    for k in range(1, nd):
        pl.semaphore_signal(barrier, inc=1, device_id=(s, lax.rem(d + k, nd)), device_id_type=MESH)
    pl.semaphore_wait(barrier, n - 1 + nd - 1)

    sent = []

    pack_slot = lax.rem(s, n_packs)
    pack_owner = (s // n_packs) == d

    def pack_copy(k):
        return remote(
            pack_ref, packs.at[pack_slot], spk.at[k], rpk.at[pack_slot], lax.rem(s + k, n), d
        )

    @pl.when(pack_owner)
    def _():
        for k in range(1, n):
            pack_copy(k).start()
        packs[pack_slot] = pack_ref[...]

    owns = (inw_ref, outw_ref)
    bufs = (win, wout)

    def start_gather(w):
        for k in range(1, n_out):
            c = remote(owns[w], bufs[w].at[s], sz.at[w, k], rz.at[w, k], outer_at(k) * n_in + q, d)
            c.start()
            sent.append(c)
        for j in range(1, n_in):
            c = remote(
                owns[w], bufs[w].at[s], sq.at[w, j, 0], rq.at[w, j, 0], a * n_in + inner_at(j), d
            )
            c.start()
            sent.append(c)
        bufs[w][s] = owns[w][...]

    def forward_gather(w):
        for k in range(1, n_out):
            src = outer_at(-k) * n_in + q
            block = bufs[w].at[src]
            remote(block, block, sz.at[w, k], rz.at[w, k], s, d).wait_recv()
            for j in range(1, n_in):
                c = remote(
                    block, block, sq.at[w, j, k], rq.at[w, j, k], a * n_in + inner_at(j), d
                )
                c.start()
                sent.append(c)

    def finish_gather(w):
        for k in range(n_out):
            for j in range(1, n_in):
                block = bufs[w].at[outer_at(-k) * n_in + inner_at(-j)]
                remote(block, block, sq.at[w, j, k], rq.at[w, j, k], s, d).wait_recv()

    start_gather(0)
    start_gather(1)
    forward_gather(0)

    for k in range(n_packs):
        source = d * n_packs + k

        @pl.when(source != s)
        def _():
            remote(packs.at[k], packs.at[k], spk.at[0], rpk.at[k], s, d).wait_recv()

    params = packs[...].reshape(total_states, LANES)

    def spread(column, lanes):
        lane = lax.broadcasted_iota(jnp.int32, (LANES, lanes), 0)
        return exact_dot(params, jnp.where(lane == column, 1.0, 0.0).astype(f32))

    def tiled(first):
        lane = lax.broadcasted_iota(jnp.int32, (LANES, own_chans), 0)
        chan = lax.broadcasted_iota(jnp.int32, (LANES, own_chans), 1)
        return exact_dot(
            params, jnp.where(lane == first + lax.rem(chan, chans), 1.0, 0.0).astype(f32)
        )

    rate, freq = spread(4 * chans, length), spread(4 * chans + 1, length)
    step = jnp.exp(spread(4 * chans + 2, length))
    gains = spread(4 * chans + 3, length)
    skips[...] = gains.reshape(n_groups, states, length)[:, :chans, :].reshape(own_chans, length)
    magnitude = jnp.exp(-rate * step)
    angle = freq * step
    ar = magnitude * jnp.cos(angle)
    ai = magnitude * jnp.sin(angle)
    modulus = rate * rate + freq * freq
    hr = ((-rate * (ar - 1.0) + freq * ai) / modulus)[:, :own_chans]
    hi = ((-freq * (ar - 1.0) - rate * ai) / modulus)[:, :own_chans]
    dr, di = tiled(0), tiled(chans)
    mine = (
        lax.broadcasted_iota(jnp.int32, (total_states, own_chans), 0) // states
        == lax.broadcasted_iota(jnp.int32, (total_states, own_chans), 1) // chans
    )
    top, bottom = pl.ds(0, total_states), pl.ds(total_states, total_states)
    btab[top] = jnp.where(mine, hr * dr - hi * di, 0.0).astype(bf16)
    btab[bottom] = jnp.where(mine, hr * di + hi * dr, 0.0).astype(bf16)
    ctab[top] = jnp.where(mine, tiled(2 * chans), 0.0).astype(bf16)
    ctab[bottom] = jnp.where(mine, -tiled(3 * chans), 0.0).astype(bf16)

    lane = lax.broadcasted_iota(jnp.int32, (total_states, length), 1)
    log_steps = max(1, (length - 1).bit_length())
    fr = br = jnp.ones((total_states, length), f32)
    fi = bi = jnp.zeros((total_states, length), f32)
    up, down = lane + 1, length - lane
    for b in range(length.bit_length()):
        if b < log_steps:
            steps[b, 0] = ar
            steps[b, 1] = ai
        hit = ((up >> b) & 1) == 1
        fr, fi = jnp.where(hit, fr * ar - fi * ai, fr), jnp.where(hit, fr * ai + fi * ar, fi)
        hit = ((down >> b) & 1) == 1
        br, bi = jnp.where(hit, br * ar - bi * ai, br), jnp.where(hit, br * ai + bi * ar, bi)
        ar, ai = ar * ar - ai * ai, 2.0 * ar * ai
    pows[0], pows[1], pows[2], pows[3] = fr, fi, br, bi

    def to_rows(column_of):
        turned = column_of.T
        return turned

    def row_blocks(matrix, at):
        turned = matrix.T[at : at + 1, :]
        return jnp.concatenate([turned[:, h * LANES : (h + 1) * LANES] for h in range(halves)], axis=0)

    jump_r, jump_i = row_blocks(fr, length - 1), row_blocks(fi, length - 1)

    def to_columns(blocks):
        parts = [
            jnp.broadcast_to(blocks[h : h + 1, :], (LANES, LANES)).T for h in range(halves)
        ]
        full = jnp.concatenate(parts, axis=0)
        return jnp.concatenate([full] * (length // LANES), axis=1) if length > LANES else full

    def scan(xr, xi, reverse):
        for b in range(log_steps):
            gap = 1 << b
            mr, mi = steps[b, 0], steps[b, 1]
            if reverse:
                mi = -mi
                keep = lane < length - gap
                shift = length - gap
            else:
                keep = lane >= gap
                shift = gap
            pr = jnp.where(keep, pltpu.roll(xr, shift, 1), 0.0)
            pi = jnp.where(keep, pltpu.roll(xi, shift, 1), 0.0)
            xr, xi = xr + mr * pr - mi * pi, xi + mr * pi + mi * pr
        return xr, xi

    def send_ends(e, xr, xi, at):
        ends_out[e, :halves] = row_blocks(xr, at)
        ends_out[e, halves:] = row_blocks(xi, at)
        for k in range(1, n):
            c = remote(
                ends_out.at[e], ends.at[e, s], sen.at[e, k], ren.at[e, k], lax.rem(s + k, n), d
            )
            c.start()
            sent.append(c)
        ends[e, s] = ends_out[e]

    def carried(e, reverse):
        for k in range(1, n):
            block = ends.at[e, lax.rem(s - k + n, n)]
            remote(block, block, sen.at[e, k], ren.at[e, k], s, d).wait_recv()
        mr = jump_r
        mi = -jump_i if reverse else jump_i
        cr = jnp.zeros((halves, LANES), f32)
        ci = jnp.zeros((halves, LANES), f32)
        for j in range(n - 1, -1, -1) if reverse else range(n):
            use = (s < j) if reverse else (s > j)
            nr = mr * cr - mi * ci + ends[e, j, :halves]
            ni = mr * ci + mi * cr + ends[e, j, halves:]
            cr, ci = jnp.where(use, nr, cr), jnp.where(use, ni, ci)
        return to_columns(cr), to_columns(ci)

    def send_partials(e, part):
        dps[e] = part.astype(bf16).reshape(nd, own_chans, length)
        for k in range(1, nd):
            other = lax.rem(d + k, nd)
            c = remote(dps.at[e, other], dpr.at[e, d], sdp.at[e, k], rdp.at[e, k], s, other)
            c.start()
            sent.append(c)
        dpr[e, d] = dps[e, d]

    def send_share(e, share):
        dpr[e, d] = share
        for k in range(1, nd):
            block = dpr.at[e, d]
            c = remote(block, block, sdp.at[e, k], rdp.at[e, k], s, lax.rem(d + k, nd))
            c.start()
            sent.append(c)

    def wait_shares(e):
        for k in range(1, nd):
            block = dpr.at[e, lax.rem(d - k + nd, nd)]
            remote(block, block, sdp.at[e, k], rdp.at[e, k], s, d).wait_recv()

    def summed(e):
        wait_shares(e)
        total = dpr[e, 0].astype(f32)
        for k in range(1, nd):
            total = total + dpr[e, k].astype(f32)
        return total.astype(bf16)

    def start_reduce(r, part):
        for block in range(n):
            rsb[r, block % n_in, block // n_in] = part[block * rows : (block + 1) * rows].astype(bf16)
        for k in list(range(1, n_out)) + [0]:
            for j in range(1, n_in):
                c = remote(
                    rsb.at[r, inner_at(j), outer_at(k)],
                    rsr.at[r, j, k],
                    srs.at[r, j, k],
                    rrs.at[r, j, k],
                    a * n_in + inner_at(j),
                    d,
                )
                c.start()
                sent.append(c)

    def inner_sum(r, k):
        total = rsb[r, q, outer_at(k)].astype(f32)
        for j in range(1, n_in):
            block = rsr.at[r, j, k]
            remote(block, block, srs.at[r, j, k], rrs.at[r, j, k], s, d).wait_recv()
            total = total + rsr[r, j, k].astype(f32)
        return total

    def forward_reduce(r):
        for k in range(1, n_out):
            zs[r, k] = inner_sum(r, k).astype(bf16)
            c = remote(
                zs.at[r, k], zr.at[r, k], szs.at[r, k], rzs.at[r, k], outer_at(k) * n_in + q, d
            )
            c.start()
            sent.append(c)

    def finish_reduce(r):
        total = inner_sum(r, 0)
        for k in range(1, n_out):
            block = zr.at[r, k]
            remote(block, block, szs.at[r, k], rzs.at[r, k], s, d).wait_recv()
            total = total + zr[r, k].astype(f32)
        return total * (n * length) ** (-0.5)

    forward_gather(1)
    finish_gather(0)
    full_in = win[...].reshape(n * rows, width)
    send_partials(0, dot_nt(full_in, tok_ref[...]))
    drive = summed(0)
    push = fast_dot(btab[...], drive)
    xr, xi = scan(push[:total_states], push[total_states:], False)
    send_ends(0, xr, xi, length - 1)

    finish_gather(1)
    send_partials(1, dot_nt(wout[...].reshape(n * rows, width), cot_ref[...]))
    back = summed(1).astype(f32)

    cr, ci = carried(0, False)
    fr, fi = pows[0], pows[1]
    xr, xi = xr + fr * cr - fi * ci, xi + fr * ci + fi * cr
    mixed = dot_tn(ctab[...], jnp.concatenate([xr, xi], axis=0).astype(bf16))
    mixed = mixed + skips[...] * drive.astype(f32)
    root = 0.7978845608028654
    squared = mixed * mixed
    bent = jnp.tanh(root * mixed * (1.0 + 0.044715 * squared))
    send_share(2, (0.5 * mixed * (1.0 + bent)).astype(bf16))
    slope = 0.5 * (1.0 + bent) + 0.5 * mixed * (1.0 - bent * bent) * root * (
        1.0 + 3.0 * 0.044715 * squared
    )
    inner = slope * back
    pulled = fast_dot(ctab[...], inner.astype(bf16))
    yr, yi = scan(pulled[:total_states], pulled[total_states:], True)
    send_ends(1, yr, yi, 0)

    wait_shares(2)
    start_reduce(0, fast_dot(dpr[2].reshape(n * rows, length), cot_ref[...]))

    cr, ci = carried(1, True)
    br, bi = pows[2], -pows[3]
    yr, yi = yr + br * cr - bi * ci, yi + br * ci + bi * cr
    grad = dot_tn(btab[...], jnp.concatenate([yr, yi], axis=0).astype(bf16))
    send_share(3, (grad + skips[...] * inner).astype(bf16))
    wait_shares(3)
    grad_cols = dpr[3].reshape(n * rows, length)
    start_reduce(1, fast_dot(grad_cols, tok_ref[...]))
    forward_reduce(0)
    gt_ref[...] = dot_tn(grad_cols, win[...].reshape(n * rows, width)).astype(bf16)
    forward_reduce(1)
    gow_ref[...] = finish_reduce(0)
    giw_ref[...] = finish_reduce(1)

    for c in sent:
        c.wait_send()

    @pl.when(pack_owner)
    def _():
        for k in range(1, n):
            pack_copy(k).wait_send()


def solution(mesh):
    n, nd = mesh.shape["sp"], mesh.shape["dp"]
    n_in = 4 if n % 4 == 0 else 1
    n_out = n // n_in

    def on_device(
        tokens,
        cotangent,
        in_weight,
        out_weight,
        decay_rate,
        frequency,
        step_log,
        drive_real,
        drive_imag,
        readout_real_part,
        readout_imaginary,
        skip_gain,
    ):
        length, width = tokens.shape
        rows = in_weight.shape[0]
        groups_here, states, chans = drive_real.shape
        n_groups = groups_here * n // nd
        n_packs = n // nd
        pack = jnp.concatenate(
            [
                drive_real,
                drive_imag,
                jnp.swapaxes(readout_real_part, 1, 2),
                jnp.swapaxes(readout_imaginary, 1, 2),
                decay_rate[..., None],
                frequency[..., None],
                jnp.broadcast_to(step_log[:, None, None], (groups_here, states, 1)),
                jnp.pad(skip_gain, ((0, 0), (0, states - chans)))[..., None],
                jnp.zeros((groups_here, states, LANES - 4 * chans - 4), f32),
            ],
            axis=2,
        ).reshape(groups_here * states, LANES)
        total_states = n_groups * states
        own_chans = n_groups * chans
        end_rows = 2 * total_states // LANES
        log_steps = max(1, (length - 1).bit_length())
        dma = pltpu.SemaphoreType.DMA
        vmem = pl.BlockSpec(memory_space=pltpu.VMEM)
        return pl.pallas_call(
            functools.partial(kernel, (n, nd, n_out, n_in, states, chans, n_groups)),
            out_shape=(
                jax.ShapeDtypeStruct((length, width), bf16),
                jax.ShapeDtypeStruct((rows, width), f32),
                jax.ShapeDtypeStruct((rows, width), f32),
            ),
            in_specs=[vmem] * 5,
            out_specs=(vmem,) * 3,
            scratch_shapes=[
                pltpu.VMEM((n, rows, width), bf16),
                pltpu.VMEM((n, rows, width), bf16),
                pltpu.VMEM((n_packs, groups_here * states, LANES), f32),
                pltpu.VMEM((2 * total_states, own_chans), bf16),
                pltpu.VMEM((2 * total_states, own_chans), bf16),
                pltpu.VMEM((log_steps, 2, total_states, length), f32),
                pltpu.VMEM((4, total_states, length), f32),
                pltpu.VMEM((own_chans, length), f32),
                pltpu.VMEM((2, nd, own_chans, length), bf16),
                pltpu.VMEM((4, nd, own_chans, length), bf16),
                pltpu.VMEM((2, end_rows, LANES), f32),
                pltpu.VMEM((2, n, end_rows, LANES), f32),
                pltpu.VMEM((2, n_in, n_out, rows, width), bf16),
                pltpu.VMEM((2, n_in, n_out, rows, width), bf16),
                pltpu.VMEM((2, n_out, rows, width), bf16),
                pltpu.VMEM((2, n_out, rows, width), bf16),
                dma((2, n_out)),
                dma((2, n_out)),
                dma((2, n_in, n_out)),
                dma((2, n_in, n_out)),
                dma((n,)),
                dma((n_packs,)),
                dma((4, nd)),
                dma((4, nd)),
                dma((2, n)),
                dma((2, n)),
                dma((2, n_in, n_out)),
                dma((2, n_in, n_out)),
                dma((2, n_out)),
                dma((2, n_out)),
            ],
            compiler_params=pltpu.CompilerParams(
                collective_id=0, has_side_effects=True, vmem_limit_bytes=48 * 1024 * 1024
            ),
        )(tokens, cotangent, in_weight, out_weight, pack)

    return jax.shard_map(
        on_device,
        mesh=mesh,
        in_specs=(
            P("sp", "dp"),
            P("sp", "dp"),
            P("sp", "dp"),
            P("sp", "dp"),
            P("sp", None),
            P("sp", None),
            P("sp"),
            P("sp", None, None),
            P("sp", None, None),
            P("sp", None, None),
            P("sp", None, None),
            P("sp", None),
        ),
        out_specs=(P("sp", "dp"), P("sp", "dp"), P("sp", "dp")),
        check_vma=False,
    )
```

```python
import functools

import jax
import jax.numpy as jnp
from jax import lax
from jax.experimental import pallas as pl
from jax.experimental.pallas import tpu as pltpu
from jax.sharding import PartitionSpec as P

MESH = pl.DeviceIdType.MESH
f32 = jnp.float32
bf16 = jnp.bfloat16
LANES = 128


def exact_dot(a, b):
    return jnp.dot(a, b, precision=lax.Precision.HIGHEST, preferred_element_type=f32)


def fast_dot(a, b):
    return jnp.dot(a, b, preferred_element_type=f32)


def exact_tn(a, b):
    return lax.dot_general(
        a,
        b,
        (((0,), (0,)), ((), ())),
        precision=lax.Precision.HIGHEST,
        preferred_element_type=f32,
    )


def dot_nt(a, b):
    return lax.dot_general(a, b, (((1,), (1,)), ((), ())), preferred_element_type=f32)


def dot_tn(a, b):
    return lax.dot_general(a, b, (((0,), (0,)), ((), ())), preferred_element_type=f32)


def kernel(
    sizes,
    tok_hbm,
    cot_hbm,
    inw_hbm,
    outw_hbm,
    rate_hbm,
    freq_hbm,
    step_ref,
    dr_hbm,
    di_hbm,
    ror_hbm,
    roi_hbm,
    skip_hbm,
    gt_ref,
    grads_ref,
    tok_ref,
    cot_ref,
    rate_ref,
    freq_ref,
    dr_ref,
    di_ref,
    ror_ref,
    roi_ref,
    skip_ref,
    pack_ref,
    win,
    wout,
    packs,
    btab,
    ctab,
    steps,
    pows,
    skips,
    dps,
    dpr,
    ends_out,
    ends,
    rsb,
    rsr,
    zs,
    zr,
    loads,
    sz,
    rz,
    sq,
    rq,
    sdp,
    rdp,
    sen,
    ren,
    srs,
    rrs,
    szs,
    rzs,
):
    n, nd, n_out, n_in, states, chans, n_groups = sizes
    length = tok_ref.shape[0]
    rows, width = inw_hbm.shape
    n_packs = packs.shape[0]
    total_states = n_groups * states
    own_chans = n_groups * chans
    halves = total_states // LANES
    s = lax.axis_index("sp")
    d = lax.axis_index("dp")
    a = s // n_in
    q = lax.rem(s, n_in)

    def remote(src, dst, ssem, rsem, sp, dp):
        return pltpu.make_async_remote_copy(
            src_ref=src,
            dst_ref=dst,
            send_sem=ssem,
            recv_sem=rsem,
            device_id=(sp, dp),
            device_id_type=MESH,
        )

    def outer_at(k):
        return lax.rem(a + k + n_out, n_out)

    def inner_at(j):
        return lax.rem(q + j + n_in, n_in)

    bufs = (win, wout)
    load_in = pltpu.make_async_copy(inw_hbm, win.at[s], loads.at[0])
    load_out = pltpu.make_async_copy(outw_hbm, wout.at[s], loads.at[1])
    load_tok = pltpu.make_async_copy(tok_hbm, tok_ref, loads.at[2])
    load_cot = pltpu.make_async_copy(cot_hbm, cot_ref, loads.at[3])
    params_in = (
        (rate_hbm, rate_ref),
        (freq_hbm, freq_ref),
        (dr_hbm, dr_ref),
        (di_hbm, di_ref),
        (ror_hbm, ror_ref),
        (roi_hbm, roi_ref),
        (skip_hbm, skip_ref),
    )
    load_params = [
        pltpu.make_async_copy(there, here, loads.at[4 + i])
        for i, (there, here) in enumerate(params_in)
    ]
    for load in load_params + [load_in, load_out, load_tok, load_cot]:
        load.start()

    barrier = pltpu.get_barrier_semaphore()
    for k in range(1, n):
        pl.semaphore_signal(barrier, inc=1, device_id=(lax.rem(s + k, n), d), device_id_type=MESH)
    for k in range(1, nd):
        pl.semaphore_signal(barrier, inc=1, device_id=(s, lax.rem(d + k, nd)), device_id_type=MESH)

    def place(count, first):
        lane = lax.broadcasted_iota(jnp.int32, (count, LANES), 1)
        return jnp.where(lane == first + lax.broadcasted_iota(jnp.int32, (count, LANES), 0), 1.0, 0.0)

    def place_row(row, column):
        spot = lax.broadcasted_iota(jnp.int32, (8, LANES), 0) == 0
        spot = spot & (lax.broadcasted_iota(jnp.int32, (8, LANES), 1) == column)
        return exact_tn(jnp.broadcast_to(row, (8, row.shape[1])), jnp.where(spot, 1.0, 0.0))

    for load in load_params:
        load.wait()
    for g in range(dr_ref.shape[0]):
        spots = [place(chans, m * chans) for m in range(4)]
        block = exact_tn(dr_ref[g], spots[0]) + exact_tn(di_ref[g], spots[1])
        block = block + exact_tn(ror_ref[g], spots[2]) + exact_tn(roi_ref[g], spots[3])
        block = block + place_row(rate_ref[g : g + 1, :], 4 * chans)
        block = block + place_row(freq_ref[g : g + 1, :], 4 * chans + 1)
        lane = lax.broadcasted_iota(jnp.int32, (states, LANES), 1)
        block = block + jnp.where(lane == 4 * chans + 2, step_ref[g], 0.0)
        gain = place_row(skip_ref[g : g + 1, :], 4 * chans + 3)
        pack_ref[g * states : g * states + chans] = block[:chans] + gain
        pack_ref[g * states + chans : (g + 1) * states] = block[chans:]
    with jax.named_scope("barrier"):
        pl.semaphore_wait(barrier, n - 1 + nd - 1)

    sent = []

    def when_used(w, src, act):
        if w == 2:
            pl.when(src // n_packs == d)(act)
        else:
            act()

    def slot(w, src):
        return packs.at[lax.rem(src, n_packs)] if w == 2 else bufs[w].at[src]

    def own(w):
        return pack_ref if w == 2 else bufs[w].at[s]

    def outer_copy(w, k):
        return remote(own(w), slot(w, s), sz.at[w, k], rz.at[w, k], outer_at(k) * n_in + q, d)

    def inner_copy(w, j, k):
        src = outer_at(-k) * n_in + q
        block = own(w) if k == 0 else slot(w, src)
        peer = a * n_in + inner_at(j)
        return remote(block, slot(w, src), sq.at[w, j, k], rq.at[w, j, k], peer, d)

    def send_outer(w):
        def act():
            for k in range(1, n_out):
                outer_copy(w, k).start()

        when_used(w, s, act)

    def send_inner(w):
        def act():
            for j in range(1, n_in):
                inner_copy(w, j, 0).start()

        when_used(w, s, act)

    def forward_gather(w):
        for k in range(1, n_out):
            src = outer_at(-k) * n_in + q

            def act():
                block = slot(w, src)
                remote(block, block, sz.at[w, k], rz.at[w, k], s, d).wait_recv()
                for j in range(1, n_in):
                    inner_copy(w, j, k).start()

            when_used(w, src, act)

    def finish_gather(w):
        for k in range(n_out):
            for j in range(1, n_in):
                src = outer_at(-k) * n_in + inner_at(-j)

                def act():
                    block = slot(w, src)
                    remote(block, block, sq.at[w, j, k], rq.at[w, j, k], s, d).wait_recv()

                when_used(w, src, act)

    def drain_gather(w):
        for k in range(n_out):

            def act():
                if k:
                    outer_copy(w, k).wait_send()

            when_used(w, s, act)

            def act():
                for j in range(1, n_in):
                    inner_copy(w, j, k).wait_send()

            when_used(w, outer_at(-k) * n_in + q, act)

    with jax.named_scope("starts"):
        send_outer(2)
        send_inner(2)
        load_in.wait()
        send_outer(0)
        send_inner(0)
        load_out.wait()
        send_outer(1)

        @pl.when(s // n_packs == d)
        def _():
            packs[lax.rem(s, n_packs)] = pack_ref[...]

    with jax.named_scope("fwd2"):
        forward_gather(2)
    with jax.named_scope("fwd0"):
        forward_gather(0)
    send_inner(1)

    with jax.named_scope("fin2"):
        finish_gather(2)
    params = packs[...].reshape(total_states, LANES)

    def spread(column, lanes):
        lane = lax.broadcasted_iota(jnp.int32, (LANES, lanes), 0)
        return exact_dot(params, jnp.where(lane == column, 1.0, 0.0).astype(f32))

    def tiled(first):
        lane = lax.broadcasted_iota(jnp.int32, (LANES, own_chans), 0)
        chan = lax.broadcasted_iota(jnp.int32, (LANES, own_chans), 1)
        return exact_dot(
            params, jnp.where(lane == first + lax.rem(chan, chans), 1.0, 0.0).astype(f32)
        )

    rate, freq = spread(4 * chans, length), spread(4 * chans + 1, length)
    step = jnp.exp(spread(4 * chans + 2, length))
    gains = spread(4 * chans + 3, length)
    skips[...] = gains.reshape(n_groups, states, length)[:, :chans, :].reshape(own_chans, length)
    magnitude = jnp.exp(-rate * step)
    angle = freq * step
    ar = magnitude * jnp.cos(angle)
    ai = magnitude * jnp.sin(angle)
    modulus = rate * rate + freq * freq
    hr = ((-rate * (ar - 1.0) + freq * ai) / modulus)[:, :own_chans]
    hi = ((-freq * (ar - 1.0) - rate * ai) / modulus)[:, :own_chans]
    dr, di = tiled(0), tiled(chans)
    mine = (
        lax.broadcasted_iota(jnp.int32, (total_states, own_chans), 0) // states
        == lax.broadcasted_iota(jnp.int32, (total_states, own_chans), 1) // chans
    )
    top, bottom = pl.ds(0, total_states), pl.ds(total_states, total_states)
    btab[top] = jnp.where(mine, hr * dr - hi * di, 0.0).astype(bf16)
    btab[bottom] = jnp.where(mine, hr * di + hi * dr, 0.0).astype(bf16)
    ctab[top] = jnp.where(mine, tiled(2 * chans), 0.0).astype(bf16)
    ctab[bottom] = jnp.where(mine, -tiled(3 * chans), 0.0).astype(bf16)

    lane = lax.broadcasted_iota(jnp.int32, (total_states, length), 1)
    log_steps = max(1, (length - 1).bit_length())
    fr = br = jnp.ones((total_states, length), f32)
    fi = bi = jnp.zeros((total_states, length), f32)
    up, down = lane + 1, length - lane
    for b in range(length.bit_length()):
        if b < log_steps:
            steps[b, 0] = ar
            steps[b, 1] = ai
        hit = ((up >> b) & 1) == 1
        fr, fi = jnp.where(hit, fr * ar - fi * ai, fr), jnp.where(hit, fr * ai + fi * ar, fi)
        hit = ((down >> b) & 1) == 1
        br, bi = jnp.where(hit, br * ar - bi * ai, br), jnp.where(hit, br * ai + bi * ar, bi)
        ar, ai = ar * ar - ai * ai, 2.0 * ar * ai
    pows[0], pows[1], pows[2], pows[3] = fr, fi, br, bi

    def row_blocks(matrix, at):
        turned = matrix.T[at : at + 1, :]
        return jnp.concatenate([turned[:, h * LANES : (h + 1) * LANES] for h in range(halves)], axis=0)

    jump_r, jump_i = row_blocks(fr, length - 1), row_blocks(fi, length - 1)

    def to_columns(blocks):
        parts = [
            jnp.broadcast_to(blocks[h : h + 1, :], (LANES, LANES)).T for h in range(halves)
        ]
        full = jnp.concatenate(parts, axis=0)
        return jnp.concatenate([full] * (length // LANES), axis=1) if length > LANES else full

    def scan(xr, xi, reverse):
        for b in range(log_steps):
            gap = 1 << b
            mr, mi = steps[b, 0], steps[b, 1]
            if reverse:
                mi = -mi
                keep = lane < length - gap
                shift = length - gap
            else:
                keep = lane >= gap
                shift = gap
            pr = jnp.where(keep, pltpu.roll(xr, shift, 1), 0.0)
            pi = jnp.where(keep, pltpu.roll(xi, shift, 1), 0.0)
            xr, xi = xr + mr * pr - mi * pi, xi + mr * pi + mi * pr
        return xr, xi

    def send_ends(e, xr, xi, at):
        ends_out[e, :halves] = row_blocks(xr, at)
        ends_out[e, halves:] = row_blocks(xi, at)
        for k in range(1, n):
            c = remote(
                ends_out.at[e], ends.at[e, s], sen.at[e, k], ren.at[e, k], lax.rem(s + k, n), d
            )
            c.start()
            sent.append(c)
        ends[e, s] = ends_out[e]

    def carried(e, reverse):
        for k in range(1, n):
            block = ends.at[e, lax.rem(s - k + n, n)]
            remote(block, block, sen.at[e, k], ren.at[e, k], s, d).wait_recv()
        mr = jump_r
        mi = -jump_i if reverse else jump_i
        cr = jnp.zeros((halves, LANES), f32)
        ci = jnp.zeros((halves, LANES), f32)
        for j in range(n - 1, -1, -1) if reverse else range(n):
            use = (s < j) if reverse else (s > j)
            nr = mr * cr - mi * ci + ends[e, j, :halves]
            ni = mr * ci + mi * cr + ends[e, j, halves:]
            cr, ci = jnp.where(use, nr, cr), jnp.where(use, ni, ci)
        return to_columns(cr), to_columns(ci)

    def send_partials(e, part):
        dps[e] = part.astype(bf16).reshape(nd, own_chans, length)
        for k in range(1, nd):
            other = lax.rem(d + k, nd)
            c = remote(dps.at[e, other], dpr.at[e, d], sdp.at[e, k], rdp.at[e, k], s, other)
            c.start()
            sent.append(c)
        dpr[e, d] = dps[e, d]

    def send_share(e, share):
        dpr[e, d] = share
        for k in range(1, nd):
            block = dpr.at[e, d]
            c = remote(block, block, sdp.at[e, k], rdp.at[e, k], s, lax.rem(d + k, nd))
            c.start()
            sent.append(c)

    def wait_shares(e):
        for k in range(1, nd):
            block = dpr.at[e, lax.rem(d - k + nd, nd)]
            remote(block, block, sdp.at[e, k], rdp.at[e, k], s, d).wait_recv()

    def summed(e):
        wait_shares(e)
        total = dpr[e, 0].astype(f32)
        for k in range(1, nd):
            total = total + dpr[e, k].astype(f32)
        return total.astype(bf16)

    def start_reduce(r, part):
        for block in range(n):
            rsb[r, block % n_in, block // n_in] = part[block * rows : (block + 1) * rows].astype(bf16)
        for k in list(range(1, n_out)) + [0]:
            for j in range(1, n_in):
                c = remote(
                    rsb.at[r, inner_at(j), outer_at(k)],
                    rsr.at[r, j, k],
                    srs.at[r, j, k],
                    rrs.at[r, j, k],
                    a * n_in + inner_at(j),
                    d,
                )
                c.start()
                sent.append(c)

    def inner_sum(r, k):
        total = rsb[r, q, outer_at(k)].astype(f32)
        for j in range(1, n_in):
            block = rsr.at[r, j, k]
            remote(block, block, srs.at[r, j, k], rrs.at[r, j, k], s, d).wait_recv()
            total = total + rsr[r, j, k].astype(f32)
        return total

    def forward_reduce(r):
        for k in range(1, n_out):
            zs[r, k] = inner_sum(r, k).astype(bf16)
            c = remote(
                zs.at[r, k], zr.at[r, k], szs.at[r, k], rzs.at[r, k], outer_at(k) * n_in + q, d
            )
            c.start()
            sent.append(c)

    def finish_reduce(r):
        total = inner_sum(r, 0)
        for k in range(1, n_out):
            block = zr.at[r, k]
            remote(block, block, szs.at[r, k], rzs.at[r, k], s, d).wait_recv()
            total = total + zr[r, k].astype(f32)
        return total

    with jax.named_scope("fwd1"):
        forward_gather(1)
    with jax.named_scope("fin0"):
        finish_gather(0)
    load_tok.wait()
    load_cot.wait()
    full_in = win[...].reshape(n * rows, width)
    with jax.named_scope("proj0"):
        send_partials(0, dot_nt(full_in, tok_ref[...]))
    with jax.named_scope("dp0"):
        drive = summed(0)
    with jax.named_scope("scan0"):
        push = fast_dot(btab[...], drive)
        xr, xi = scan(push[:total_states], push[total_states:], False)
        send_ends(0, xr, xi, length - 1)

    with jax.named_scope("fin1"):
        finish_gather(1)
    with jax.named_scope("proj1"):
        send_partials(1, dot_nt(wout[...].reshape(n * rows, width), cot_ref[...]))
    with jax.named_scope("dp1"):
        back = summed(1).astype(f32)

    with jax.named_scope("carry0"):
        cr, ci = carried(0, False)
    fr, fi = pows[0], pows[1]
    xr, xi = xr + fr * cr - fi * ci, xi + fr * ci + fi * cr
    mixed = dot_tn(ctab[...], jnp.concatenate([xr, xi], axis=0).astype(bf16))
    mixed = mixed + skips[...] * drive.astype(f32)
    root = 0.7978845608028654
    squared = mixed * mixed
    bent = jnp.tanh(root * mixed * (1.0 + 0.044715 * squared))
    send_share(2, (0.5 * mixed * (1.0 + bent)).astype(bf16))
    slope = 0.5 * (1.0 + bent) + 0.5 * mixed * (1.0 - bent * bent) * root * (
        1.0 + 3.0 * 0.044715 * squared
    )
    inner = slope * back
    pulled = fast_dot(ctab[...], inner.astype(bf16))
    yr, yi = scan(pulled[:total_states], pulled[total_states:], True)
    send_ends(1, yr, yi, 0)

    with jax.named_scope("dp2"):
        wait_shares(2)
    with jax.named_scope("rs0"):
        start_reduce(0, fast_dot(dpr[2].reshape(n * rows, length), cot_ref[...]))

    with jax.named_scope("carry1"):
        cr, ci = carried(1, True)
    br, bi = pows[2], -pows[3]
    yr, yi = yr + br * cr - bi * ci, yi + br * ci + bi * cr
    grad = dot_tn(btab[...], jnp.concatenate([yr, yi], axis=0).astype(bf16))
    send_share(3, (grad + skips[...] * inner).astype(bf16))
    with jax.named_scope("dp3"):
        wait_shares(3)
    grad_cols = dpr[3].reshape(n * rows, length)
    with jax.named_scope("rs1"):
        start_reduce(1, fast_dot(grad_cols, tok_ref[...]))
    with jax.named_scope("frs0"):
        forward_reduce(0)
    with jax.named_scope("gt"):
        gt_ref[...] = dot_tn(grad_cols, win[...].reshape(n * rows, width)).astype(bf16)
    with jax.named_scope("frs1"):
        forward_reduce(1)
    with jax.named_scope("fin_rs0"):
        grads_ref[1] = finish_reduce(0)
    with jax.named_scope("fin_rs1"):
        grads_ref[0] = finish_reduce(1)

    for c in sent:
        c.wait_send()

    for w in range(3):
        drain_gather(w)


def solution(mesh):
    n, nd = mesh.shape["sp"], mesh.shape["dp"]
    n_in = 4 if n % 4 == 0 else 1
    n_out = n // n_in

    def on_device(
        tokens,
        cotangent,
        in_weight,
        out_weight,
        decay_rate,
        frequency,
        step_log,
        drive_real,
        drive_imag,
        readout_real_part,
        readout_imaginary,
        skip_gain,
    ):
        length, width = tokens.shape
        rows = in_weight.shape[0]
        groups_here, states, chans = drive_real.shape
        n_groups = groups_here * n // nd
        n_packs = n // nd
        total_states = n_groups * states
        own_chans = n_groups * chans
        end_rows = 2 * total_states // LANES
        log_steps = max(1, (length - 1).bit_length())
        dma = pltpu.SemaphoreType.DMA
        vmem = pl.BlockSpec(memory_space=pltpu.VMEM)
        anywhere = pl.BlockSpec(memory_space=pl.ANY)
        scale = (n * length) ** (-0.5)
        grad_tokens, grads = pl.pallas_call(
            functools.partial(kernel, (n, nd, n_out, n_in, states, chans, n_groups)),
            out_shape=(
                pltpu.VMEM((length, width), bf16),
                pltpu.VMEM((2, rows, width), f32),
            ),
            in_specs=[anywhere] * 6 + [pl.BlockSpec(memory_space=pltpu.SMEM)] + [anywhere] * 5,
            out_specs=(vmem,) * 2,
            scratch_shapes=[
                pltpu.VMEM((length, width), bf16),
                pltpu.VMEM((length, width), bf16),
                pltpu.VMEM((groups_here, states), f32),
                pltpu.VMEM((groups_here, states), f32),
                pltpu.VMEM((groups_here, chans, states), f32),
                pltpu.VMEM((groups_here, chans, states), f32),
                pltpu.VMEM((groups_here, chans, states), f32),
                pltpu.VMEM((groups_here, chans, states), f32),
                pltpu.VMEM((groups_here, chans), f32),
                pltpu.VMEM((groups_here * states, LANES), f32),
                pltpu.VMEM((n, rows, width), bf16),
                pltpu.VMEM((n, rows, width), bf16),
                pltpu.VMEM((n_packs, groups_here * states, LANES), f32),
                pltpu.VMEM((2 * total_states, own_chans), bf16),
                pltpu.VMEM((2 * total_states, own_chans), bf16),
                pltpu.VMEM((log_steps, 2, total_states, length), f32),
                pltpu.VMEM((4, total_states, length), f32),
                pltpu.VMEM((own_chans, length), f32),
                pltpu.VMEM((2, nd, own_chans, length), bf16),
                pltpu.VMEM((4, nd, own_chans, length), bf16),
                pltpu.VMEM((2, end_rows, LANES), f32),
                pltpu.VMEM((2, n, end_rows, LANES), f32),
                pltpu.VMEM((2, n_in, n_out, rows, width), bf16),
                pltpu.VMEM((2, n_in, n_out, rows, width), bf16),
                pltpu.VMEM((2, n_out, rows, width), bf16),
                pltpu.VMEM((2, n_out, rows, width), bf16),
                dma((11,)),
                dma((3, n_out)),
                dma((3, n_out)),
                dma((3, n_in, n_out)),
                dma((3, n_in, n_out)),
                dma((4, nd)),
                dma((4, nd)),
                dma((2, n)),
                dma((2, n)),
                dma((2, n_in, n_out)),
                dma((2, n_in, n_out)),
                dma((2, n_out)),
                dma((2, n_out)),
            ],
            compiler_params=pltpu.CompilerParams(
                collective_id=0, has_side_effects=True, vmem_limit_bytes=67043328 - 4 * 1024 * 1024
            ),
        )(
            tokens,
            cotangent,
            in_weight,
            out_weight,
            decay_rate,
            frequency,
            step_log,
            jnp.swapaxes(drive_real, 1, 2),
            jnp.swapaxes(drive_imag, 1, 2),
            readout_real_part,
            readout_imaginary,
            skip_gain,
        )
        return grad_tokens, grads[0] * scale, grads[1] * scale

    return jax.shard_map(
        on_device,
        mesh=mesh,
        in_specs=(
            P("sp", "dp"),
            P("sp", "dp"),
            P("sp", "dp"),
            P("sp", "dp"),
            P("sp", None),
            P("sp", None),
            P("sp"),
            P("sp", None, None),
            P("sp", None, None),
            P("sp", None, None),
            P("sp", None, None),
            P("sp", None),
        ),
        out_specs=(P("sp", "dp"), P("sp", "dp"), P("sp", "dp")),
        check_vma=False,
    )
```

```python
import functools

import jax
import jax.numpy as jnp
from jax import lax
from jax.experimental import pallas as pl
from jax.experimental.pallas import tpu as pltpu
from jax.sharding import PartitionSpec as P

MESH = pl.DeviceIdType.MESH
f32 = jnp.float32
bf16 = jnp.bfloat16
LANES = 128


def exact_dot(a, b):
    return jnp.dot(a, b, precision=lax.Precision.HIGHEST, preferred_element_type=f32)


def fast_dot(a, b):
    return jnp.dot(a, b, preferred_element_type=f32)


def exact_tn(a, b):
    return lax.dot_general(
        a,
        b,
        (((0,), (0,)), ((), ())),
        precision=lax.Precision.HIGHEST,
        preferred_element_type=f32,
    )


def dot_nt(a, b):
    return lax.dot_general(a, b, (((1,), (1,)), ((), ())), preferred_element_type=f32)


def dot_tn(a, b):
    return lax.dot_general(a, b, (((0,), (0,)), ((), ())), preferred_element_type=f32)


def kernel(
    sizes,
    tok_hbm,
    cot_hbm,
    inw_hbm,
    outw_hbm,
    rate_hbm,
    freq_hbm,
    step_ref,
    dr_hbm,
    di_hbm,
    ror_hbm,
    roi_hbm,
    skip_hbm,
    gt_ref,
    grads_ref,
    tok_ref,
    cot_ref,
    rate_ref,
    freq_ref,
    dr_ref,
    di_ref,
    ror_ref,
    roi_ref,
    skip_ref,
    pack_ref,
    win,
    wout,
    packs,
    btab,
    ctab,
    steps,
    pows,
    skips,
    dps,
    dpr,
    ends_out,
    ends,
    rsb,
    rsr,
    zs,
    zr,
    loads,
    sz,
    rz,
    sq,
    rq,
    sdp,
    rdp,
    sen,
    ren,
    srs,
    rrs,
    szs,
    rzs,
):
    n, nd, n_out, n_in, states, chans, n_groups = sizes
    length = tok_ref.shape[0]
    rows, width = inw_hbm.shape
    n_packs = packs.shape[0]
    total_states = n_groups * states
    own_chans = n_groups * chans
    halves = total_states // LANES
    s = lax.axis_index("sp")
    d = lax.axis_index("dp")
    a = s // n_in
    q = lax.rem(s, n_in)

    def remote(src, dst, ssem, rsem, sp, dp):
        return pltpu.make_async_remote_copy(
            src_ref=src,
            dst_ref=dst,
            send_sem=ssem,
            recv_sem=rsem,
            device_id=(sp, dp),
            device_id_type=MESH,
        )

    def outer_at(k):
        return lax.rem(a + k + n_out, n_out)

    def inner_at(j):
        return lax.rem(q + j + n_in, n_in)

    bufs = (win, wout)
    load_in = pltpu.make_async_copy(inw_hbm, win.at[s], loads.at[0])
    load_out = pltpu.make_async_copy(outw_hbm, wout.at[s], loads.at[1])
    load_tok = pltpu.make_async_copy(tok_hbm, tok_ref, loads.at[2])
    load_cot = pltpu.make_async_copy(cot_hbm, cot_ref, loads.at[3])
    params_in = (
        (rate_hbm, rate_ref),
        (freq_hbm, freq_ref),
        (dr_hbm, dr_ref),
        (di_hbm, di_ref),
        (ror_hbm, ror_ref),
        (roi_hbm, roi_ref),
        (skip_hbm, skip_ref),
    )
    load_params = [
        pltpu.make_async_copy(there, here, loads.at[4 + i])
        for i, (there, here) in enumerate(params_in)
    ]
    for load in load_params + [load_in, load_out, load_tok, load_cot]:
        load.start()

    barrier = pltpu.get_barrier_semaphore()
    for k in range(1, n):
        pl.semaphore_signal(barrier, inc=1, device_id=(lax.rem(s + k, n), d), device_id_type=MESH)
    for k in range(1, nd):
        pl.semaphore_signal(barrier, inc=1, device_id=(s, lax.rem(d + k, nd)), device_id_type=MESH)

    def place(count, first):
        lane = lax.broadcasted_iota(jnp.int32, (count, LANES), 1)
        return jnp.where(lane == first + lax.broadcasted_iota(jnp.int32, (count, LANES), 0), 1.0, 0.0)

    def place_row(row, column):
        spot = lax.broadcasted_iota(jnp.int32, (8, LANES), 0) == 0
        spot = spot & (lax.broadcasted_iota(jnp.int32, (8, LANES), 1) == column)
        return exact_tn(jnp.broadcast_to(row, (8, row.shape[1])), jnp.where(spot, 1.0, 0.0))

    for load in load_params:
        load.wait()
    for g in range(dr_ref.shape[0]):
        spots = [place(chans, m * chans) for m in range(4)]
        block = exact_tn(dr_ref[g], spots[0]) + exact_tn(di_ref[g], spots[1])
        block = block + exact_tn(ror_ref[g], spots[2]) + exact_tn(roi_ref[g], spots[3])
        block = block + place_row(rate_ref[g : g + 1, :], 4 * chans)
        block = block + place_row(freq_ref[g : g + 1, :], 4 * chans + 1)
        lane = lax.broadcasted_iota(jnp.int32, (states, LANES), 1)
        block = block + jnp.where(lane == 4 * chans + 2, step_ref[g], 0.0)
        gain = place_row(skip_ref[g : g + 1, :], 4 * chans + 3)
        pack_ref[g * states : g * states + chans] = block[:chans] + gain
        pack_ref[g * states + chans : (g + 1) * states] = block[chans:]
    with jax.named_scope("barrier"):
        pl.semaphore_wait(barrier, n - 1 + nd - 1)

    sent = []

    def when_used(w, src, act):
        if w == 2:
            pl.when(src // n_packs == d)(act)
        else:
            act()

    def slot(w, src):
        return packs.at[lax.rem(src, n_packs)] if w == 2 else bufs[w].at[src]

    def own(w):
        return pack_ref if w == 2 else bufs[w].at[s]

    def outer_copy(w, k):
        return remote(own(w), slot(w, s), sz.at[w, k], rz.at[w, k], outer_at(k) * n_in + q, d)

    def inner_copy(w, j, k):
        src = outer_at(-k) * n_in + q
        block = own(w) if k == 0 else slot(w, src)
        peer = a * n_in + inner_at(j)
        return remote(block, slot(w, src), sq.at[w, j, k], rq.at[w, j, k], peer, d)

    def send_outer(w):
        def act():
            for k in range(1, n_out):
                outer_copy(w, k).start()

        when_used(w, s, act)

    def send_inner(w):
        def act():
            for j in range(1, n_in):
                inner_copy(w, j, 0).start()

        when_used(w, s, act)

    def forward_gather(w):
        for k in range(1, n_out):
            src = outer_at(-k) * n_in + q

            def act():
                block = slot(w, src)
                remote(block, block, sz.at[w, k], rz.at[w, k], s, d).wait_recv()
                for j in range(1, n_in):
                    inner_copy(w, j, k).start()

            when_used(w, src, act)

    def finish_gather(w):
        for k in range(n_out):
            for j in range(1, n_in):
                src = outer_at(-k) * n_in + inner_at(-j)

                def act():
                    block = slot(w, src)
                    remote(block, block, sq.at[w, j, k], rq.at[w, j, k], s, d).wait_recv()

                when_used(w, src, act)

    def drain_gather(w):
        for k in range(n_out):

            def act():
                if k:
                    outer_copy(w, k).wait_send()

            when_used(w, s, act)

            def act():
                for j in range(1, n_in):
                    inner_copy(w, j, k).wait_send()

            when_used(w, outer_at(-k) * n_in + q, act)

    with jax.named_scope("starts"):
        send_outer(2)
        send_inner(2)
        load_in.wait()
        send_outer(0)
        send_inner(0)
        load_out.wait()
        send_outer(1)

        @pl.when(s // n_packs == d)
        def _():
            packs[lax.rem(s, n_packs)] = pack_ref[...]

    with jax.named_scope("fwd2"):
        forward_gather(2)
    with jax.named_scope("fwd0"):
        forward_gather(0)
    send_inner(1)

    with jax.named_scope("fin2"):
        finish_gather(2)
    params = packs[...].reshape(total_states, LANES)

    def spread(column, lanes):
        lane = lax.broadcasted_iota(jnp.int32, (LANES, lanes), 0)
        return exact_dot(params, jnp.where(lane == column, 1.0, 0.0).astype(f32))

    def tiled(first):
        lane = lax.broadcasted_iota(jnp.int32, (LANES, own_chans), 0)
        chan = lax.broadcasted_iota(jnp.int32, (LANES, own_chans), 1)
        return exact_dot(
            params, jnp.where(lane == first + lax.rem(chan, chans), 1.0, 0.0).astype(f32)
        )

    rate, freq = spread(4 * chans, length), spread(4 * chans + 1, length)
    step = jnp.exp(spread(4 * chans + 2, length))
    gains = spread(4 * chans + 3, length)
    skips[...] = gains.reshape(n_groups, states, length)[:, :chans, :].reshape(own_chans, length)
    magnitude = jnp.exp(-rate * step)
    angle = freq * step
    ar = magnitude * jnp.cos(angle)
    ai = magnitude * jnp.sin(angle)
    modulus = rate * rate + freq * freq
    hr = ((-rate * (ar - 1.0) + freq * ai) / modulus)[:, :own_chans]
    hi = ((-freq * (ar - 1.0) - rate * ai) / modulus)[:, :own_chans]
    dr, di = tiled(0), tiled(chans)
    mine = (
        lax.broadcasted_iota(jnp.int32, (total_states, own_chans), 0) // states
        == lax.broadcasted_iota(jnp.int32, (total_states, own_chans), 1) // chans
    )
    top, bottom = pl.ds(0, total_states), pl.ds(total_states, total_states)
    btab[top] = jnp.where(mine, hr * dr - hi * di, 0.0).astype(bf16)
    btab[bottom] = jnp.where(mine, hr * di + hi * dr, 0.0).astype(bf16)
    ctab[top] = jnp.where(mine, tiled(2 * chans), 0.0).astype(bf16)
    ctab[bottom] = jnp.where(mine, -tiled(3 * chans), 0.0).astype(bf16)

    with jax.named_scope("fwd1"):
        forward_gather(1)
    lane = lax.broadcasted_iota(jnp.int32, (total_states, length), 1)
    log_steps = max(1, (length - 1).bit_length())
    fr = br = jnp.ones((total_states, length), f32)
    fi = bi = jnp.zeros((total_states, length), f32)
    up, down = lane + 1, length - lane
    for b in range(length.bit_length()):
        if b < log_steps:
            steps[b, 0] = ar
            steps[b, 1] = ai
        hit = ((up >> b) & 1) == 1
        fr, fi = jnp.where(hit, fr * ar - fi * ai, fr), jnp.where(hit, fr * ai + fi * ar, fi)
        hit = ((down >> b) & 1) == 1
        br, bi = jnp.where(hit, br * ar - bi * ai, br), jnp.where(hit, br * ai + bi * ar, bi)
        ar, ai = ar * ar - ai * ai, 2.0 * ar * ai
    pows[0], pows[1], pows[2], pows[3] = fr, fi, br, bi

    def row_blocks(matrix, at):
        turned = matrix.T[at : at + 1, :]
        return jnp.concatenate([turned[:, h * LANES : (h + 1) * LANES] for h in range(halves)], axis=0)

    jump_r, jump_i = row_blocks(fr, length - 1), row_blocks(fi, length - 1)

    def to_columns(blocks):
        parts = [
            jnp.broadcast_to(blocks[h : h + 1, :], (LANES, LANES)).T for h in range(halves)
        ]
        full = jnp.concatenate(parts, axis=0)
        return jnp.concatenate([full] * (length // LANES), axis=1) if length > LANES else full

    def scan(xr, xi, reverse):
        for b in range(log_steps):
            gap = 1 << b
            mr, mi = steps[b, 0], steps[b, 1]
            if reverse:
                mi = -mi
                keep = lane < length - gap
                shift = length - gap
            else:
                keep = lane >= gap
                shift = gap
            pr = jnp.where(keep, pltpu.roll(xr, shift, 1), 0.0)
            pi = jnp.where(keep, pltpu.roll(xi, shift, 1), 0.0)
            xr, xi = xr + mr * pr - mi * pi, xi + mr * pi + mi * pr
        return xr, xi

    def send_ends(e, xr, xi, at):
        ends_out[e, :halves] = row_blocks(xr, at)
        ends_out[e, halves:] = row_blocks(xi, at)
        for k in range(1, n):
            c = remote(
                ends_out.at[e], ends.at[e, s], sen.at[e, k], ren.at[e, k], lax.rem(s + k, n), d
            )
            c.start()
            sent.append(c)
        ends[e, s] = ends_out[e]

    def carried(e, reverse):
        for k in range(1, n):
            block = ends.at[e, lax.rem(s - k + n, n)]
            remote(block, block, sen.at[e, k], ren.at[e, k], s, d).wait_recv()
        mr = jump_r
        mi = -jump_i if reverse else jump_i
        cr = jnp.zeros((halves, LANES), f32)
        ci = jnp.zeros((halves, LANES), f32)
        for j in range(n - 1, -1, -1) if reverse else range(n):
            use = (s < j) if reverse else (s > j)
            nr = mr * cr - mi * ci + ends[e, j, :halves]
            ni = mr * ci + mi * cr + ends[e, j, halves:]
            cr, ci = jnp.where(use, nr, cr), jnp.where(use, ni, ci)
        return to_columns(cr), to_columns(ci)

    def send_partials(e, part):
        dps[e] = part.astype(bf16).reshape(nd, own_chans, length)
        for k in range(1, nd):
            other = lax.rem(d + k, nd)
            c = remote(dps.at[e, other], dpr.at[e, d], sdp.at[e, k], rdp.at[e, k], s, other)
            c.start()
            sent.append(c)
        dpr[e, d] = dps[e, d]

    def send_share(e, share):
        dpr[e, d] = share
        for k in range(1, nd):
            block = dpr.at[e, d]
            c = remote(block, block, sdp.at[e, k], rdp.at[e, k], s, lax.rem(d + k, nd))
            c.start()
            sent.append(c)

    def wait_shares(e):
        for k in range(1, nd):
            block = dpr.at[e, lax.rem(d - k + nd, nd)]
            remote(block, block, sdp.at[e, k], rdp.at[e, k], s, d).wait_recv()

    def summed(e):
        wait_shares(e)
        total = dpr[e, 0].astype(f32)
        for k in range(1, nd):
            total = total + dpr[e, k].astype(f32)
        return total.astype(bf16)

    def start_reduce(r, part):
        for block in range(n):
            rsb[r, block % n_in, block // n_in] = part[block * rows : (block + 1) * rows].astype(bf16)
        for k in list(range(1, n_out)) + [0]:
            for j in range(1, n_in):
                c = remote(
                    rsb.at[r, inner_at(j), outer_at(k)],
                    rsr.at[r, j, k],
                    srs.at[r, j, k],
                    rrs.at[r, j, k],
                    a * n_in + inner_at(j),
                    d,
                )
                c.start()
                sent.append(c)

    def inner_sum(r, k):
        total = rsb[r, q, outer_at(k)].astype(f32)
        for j in range(1, n_in):
            block = rsr.at[r, j, k]
            remote(block, block, srs.at[r, j, k], rrs.at[r, j, k], s, d).wait_recv()
            total = total + rsr[r, j, k].astype(f32)
        return total

    def forward_reduce(r):
        for k in range(1, n_out):
            zs[r, k] = inner_sum(r, k).astype(bf16)
            c = remote(
                zs.at[r, k], zr.at[r, k], szs.at[r, k], rzs.at[r, k], outer_at(k) * n_in + q, d
            )
            c.start()
            sent.append(c)

    def finish_reduce(r):
        total = inner_sum(r, 0)
        for k in range(1, n_out):
            block = zr.at[r, k]
            remote(block, block, szs.at[r, k], rzs.at[r, k], s, d).wait_recv()
            total = total + zr[r, k].astype(f32)
        return total

    with jax.named_scope("fin0"):
        finish_gather(0)
    load_tok.wait()
    load_cot.wait()
    full_in = win[...].reshape(n * rows, width)
    with jax.named_scope("proj0"):
        send_partials(0, dot_nt(full_in, tok_ref[...]))
    with jax.named_scope("dp0"):
        drive = summed(0)
    with jax.named_scope("scan0"):
        push = fast_dot(btab[...], drive)
        xr, xi = scan(push[:total_states], push[total_states:], False)
        send_ends(0, xr, xi, length - 1)

    with jax.named_scope("fin1"):
        finish_gather(1)
    with jax.named_scope("proj1"):
        send_partials(1, dot_nt(wout[...].reshape(n * rows, width), cot_ref[...]))
    with jax.named_scope("dp1"):
        back = summed(1).astype(f32)

    with jax.named_scope("carry0"):
        cr, ci = carried(0, False)
    fr, fi = pows[0], pows[1]
    xr, xi = xr + fr * cr - fi * ci, xi + fr * ci + fi * cr
    mixed = dot_tn(ctab[...], jnp.concatenate([xr, xi], axis=0).astype(bf16))
    mixed = mixed + skips[...] * drive.astype(f32)
    root = 0.7978845608028654
    squared = mixed * mixed
    bent = jnp.tanh(root * mixed * (1.0 + 0.044715 * squared))
    send_share(2, (0.5 * mixed * (1.0 + bent)).astype(bf16))
    slope = 0.5 * (1.0 + bent) + 0.5 * mixed * (1.0 - bent * bent) * root * (
        1.0 + 3.0 * 0.044715 * squared
    )
    inner = slope * back
    pulled = fast_dot(ctab[...], inner.astype(bf16))
    yr, yi = scan(pulled[:total_states], pulled[total_states:], True)
    send_ends(1, yr, yi, 0)

    with jax.named_scope("dp2"):
        wait_shares(2)
    with jax.named_scope("rs0"):
        start_reduce(0, fast_dot(dpr[2].reshape(n * rows, length), cot_ref[...]))

    with jax.named_scope("carry1"):
        cr, ci = carried(1, True)
    br, bi = pows[2], -pows[3]
    yr, yi = yr + br * cr - bi * ci, yi + br * ci + bi * cr
    grad = dot_tn(btab[...], jnp.concatenate([yr, yi], axis=0).astype(bf16))
    send_share(3, (grad + skips[...] * inner).astype(bf16))
    with jax.named_scope("dp3"):
        wait_shares(3)
    grad_cols = dpr[3].reshape(n * rows, length)
    with jax.named_scope("rs1"):
        start_reduce(1, fast_dot(grad_cols, tok_ref[...]))
    with jax.named_scope("frs0"):
        forward_reduce(0)
    with jax.named_scope("gt"):
        gt_ref[...] = dot_tn(grad_cols, win[...].reshape(n * rows, width)).astype(bf16)
    with jax.named_scope("frs1"):
        forward_reduce(1)
    with jax.named_scope("fin_rs0"):
        grads_ref[1] = finish_reduce(0)
    with jax.named_scope("fin_rs1"):
        grads_ref[0] = finish_reduce(1)

    for c in sent:
        c.wait_send()

    for w in range(3):
        drain_gather(w)


def solution(mesh):
    n, nd = mesh.shape["sp"], mesh.shape["dp"]
    n_in = 4 if n % 4 == 0 else 1
    n_out = n // n_in

    def on_device(
        tokens,
        cotangent,
        in_weight,
        out_weight,
        decay_rate,
        frequency,
        step_log,
        drive_real,
        drive_imag,
        readout_real_part,
        readout_imaginary,
        skip_gain,
    ):
        length, width = tokens.shape
        rows = in_weight.shape[0]
        groups_here, states, chans = drive_real.shape
        n_groups = groups_here * n // nd
        n_packs = n // nd
        total_states = n_groups * states
        own_chans = n_groups * chans
        end_rows = 2 * total_states // LANES
        log_steps = max(1, (length - 1).bit_length())
        dma = pltpu.SemaphoreType.DMA
        vmem = pl.BlockSpec(memory_space=pltpu.VMEM)
        anywhere = pl.BlockSpec(memory_space=pl.ANY)
        scale = (n * length) ** (-0.5)
        grad_tokens, grads = pl.pallas_call(
            functools.partial(kernel, (n, nd, n_out, n_in, states, chans, n_groups)),
            out_shape=(
                pltpu.VMEM((length, width), bf16),
                pltpu.VMEM((2, rows, width), f32),
            ),
            in_specs=[anywhere] * 6 + [pl.BlockSpec(memory_space=pltpu.SMEM)] + [anywhere] * 5,
            out_specs=(vmem,) * 2,
            scratch_shapes=[
                pltpu.VMEM((length, width), bf16),
                pltpu.VMEM((length, width), bf16),
                pltpu.VMEM((groups_here, states), f32),
                pltpu.VMEM((groups_here, states), f32),
                pltpu.VMEM((groups_here, chans, states), f32),
                pltpu.VMEM((groups_here, chans, states), f32),
                pltpu.VMEM((groups_here, chans, states), f32),
                pltpu.VMEM((groups_here, chans, states), f32),
                pltpu.VMEM((groups_here, chans), f32),
                pltpu.VMEM((groups_here * states, LANES), f32),
                pltpu.VMEM((n, rows, width), bf16),
                pltpu.VMEM((n, rows, width), bf16),
                pltpu.VMEM((n_packs, groups_here * states, LANES), f32),
                pltpu.VMEM((2 * total_states, own_chans), bf16),
                pltpu.VMEM((2 * total_states, own_chans), bf16),
                pltpu.VMEM((log_steps, 2, total_states, length), f32),
                pltpu.VMEM((4, total_states, length), f32),
                pltpu.VMEM((own_chans, length), f32),
                pltpu.VMEM((2, nd, own_chans, length), bf16),
                pltpu.VMEM((4, nd, own_chans, length), bf16),
                pltpu.VMEM((2, end_rows, LANES), f32),
                pltpu.VMEM((2, n, end_rows, LANES), f32),
                pltpu.VMEM((2, n_in, n_out, rows, width), bf16),
                pltpu.VMEM((2, n_in, n_out, rows, width), bf16),
                pltpu.VMEM((2, n_out, rows, width), bf16),
                pltpu.VMEM((2, n_out, rows, width), bf16),
                dma((11,)),
                dma((3, n_out)),
                dma((3, n_out)),
                dma((3, n_in, n_out)),
                dma((3, n_in, n_out)),
                dma((4, nd)),
                dma((4, nd)),
                dma((2, n)),
                dma((2, n)),
                dma((2, n_in, n_out)),
                dma((2, n_in, n_out)),
                dma((2, n_out)),
                dma((2, n_out)),
            ],
            compiler_params=pltpu.CompilerParams(
                collective_id=0, has_side_effects=True, vmem_limit_bytes=67043328 - 4 * 1024 * 1024
            ),
        )(
            tokens,
            cotangent,
            in_weight,
            out_weight,
            decay_rate,
            frequency,
            step_log,
            jnp.swapaxes(drive_real, 1, 2),
            jnp.swapaxes(drive_imag, 1, 2),
            readout_real_part,
            readout_imaginary,
            skip_gain,
        )
        return grad_tokens, grads[0] * scale, grads[1] * scale

    return jax.shard_map(
        on_device,
        mesh=mesh,
        in_specs=(
            P("sp", "dp"),
            P("sp", "dp"),
            P("sp", "dp"),
            P("sp", "dp"),
            P("sp", None),
            P("sp", None),
            P("sp"),
            P("sp", None, None),
            P("sp", None, None),
            P("sp", None, None),
            P("sp", None, None),
            P("sp", None),
        ),
        out_specs=(P("sp", "dp"), P("sp", "dp"), P("sp", "dp")),
        check_vma=False,
    )
```
